32 devices in a mesh: fs: 8 (over z, y), tp: 4 (over x, core).
Axes of the slice: x: 2, y: 2, z: 4, core: 2. Of those that a mesh axis runs over, the one named last changes fastest.
Arguments:
- tokens: bfloat16 [6144, 2048], P(('fs', 'tp')), may hold values from -60 to 60
- norm_gain: float32 [2048], P('fs'), may hold values from 0.1 to 1.9
- gate_weight: float32 [2048, 5632], P('fs', 'tp'), may hold values from -0.125 to 0.125
- up_weight: float32 [2048, 5632], P('fs', 'tp'), may hold values from -0.125 to 0.125
- down_weight: float32 [2048, 5632], P('fs', 'tp'), may hold values from -0.078125 to 0.078125
Outputs:
- mixed_rows: bfloat16 [6144, 2048], P(('fs', 'tp'))
- gate_out: bfloat16 [2048, 5632], P(None, 'tp')
- up_out: bfloat16 [2048, 5632], P(None, 'tp')
- down_out: bfloat16 [2048, 5632], P(None, 'tp')
The draws below stay inside these ranges and needn't reach their ends.
All inputs are finite; a program needn't handle non-finite values.
Results may differ from the reference program's by a relative error of at most 0.014.
Values may be sent and summed in bfloat16 or wider, within the bound.
A program may use at most 128 MiB of HBM per device.

```python
import math
import jax
import jax.numpy as jnp
from jax import lax

D = 2048
FF = 5632
TOKENS = 6144
N_TP = 4


def draw_tokens(key, part):
    key_base = jax.random.fold_in(key, 11)
    key_scale = jax.random.fold_in(key, 12)
    standard = jnp.clip(jax.random.normal(key_base, (TOKENS, D), jnp.float32), -6.0, 6.0)
    scales = jnp.exp(jax.random.uniform(key_scale, (TOKENS, 1), jnp.float32, math.log(0.3), math.log(3.0)))
    return (standard * scales).astype(jnp.bfloat16)


def levels(stream_key, dims, shards, low, largest):
    level = 1.0
    for axis_at, shards_of in shards:
        draws = jax.random.uniform(jax.random.fold_in(jax.random.fold_in(stream_key, 6), axis_at), (shards_of,), jnp.float32, low / len(shards), largest / len(shards))
        level = level * jnp.repeat(jnp.exp(draws), dims[axis_at] // shards_of).reshape((-1,) + (1,) * (len(dims) - 1 - axis_at))
    return level


def bell_draw(key, dims, scale, bound, pieces=(), kind=jnp.bfloat16):
    entries = scale * jax.random.normal(key, dims, jnp.float32)
    if pieces:
        entries = entries * levels(key, dims, pieces, -0.22, 0.18)
    return jnp.clip(entries, -bound, bound).astype(kind)


def setup_inputs(seed: int = 0) -> dict:
    splits = jax.random.split(jax.random.key(seed), 6)
    return {
        "tokens": draw_tokens(jax.random.fold_in(splits[5], 71), 0),
        "norm_gain": jnp.clip(1.0 + 0.18 * jax.random.normal(splits[1], (D,), jnp.float32), 0.1, 1.9),
        "gate_weight": bell_draw(splits[2], (D, FF), D ** -0.5, 0.125, ((0, 8), (1, 4)), jnp.float32),
        "up_weight": bell_draw(splits[3], (D, FF), D ** -0.5, 0.125, ((0, 8), (1, 4)), jnp.float32),
        "down_weight": bell_draw(splits[4], (D, FF), FF ** -0.5, 0.078125, ((0, 8), (1, 4)), jnp.float32),
    }


def reference(tokens, norm_gain, gate_weight, up_weight, down_weight):
    row_gain = norm_gain[:, None]
    gate_out = (gate_weight * row_gain).astype(jnp.bfloat16)
    up_out = (up_weight * row_gain).astype(jnp.bfloat16)
    down_out = down_weight.astype(jnp.bfloat16)
    widened = tokens.astype(jnp.float32)
    normed = (widened * lax.rsqrt(lax.optimization_barrier(jnp.mean(widened * widened, axis=1, keepdims=True)) + 1e-06)).astype(jnp.bfloat16)
    gate_pre = jnp.dot(normed, gate_out, preferred_element_type=jnp.float32)
    up_pre = jnp.dot(normed, up_out, preferred_element_type=jnp.float32)
    hidden = (jax.nn.silu(gate_pre) * up_pre).astype(jnp.bfloat16)
    block_width = FF // N_TP
    running = jnp.zeros((tokens.shape[0], D), jnp.float32)
    for block in range(N_TP):
        lower = block * block_width
        partial_value = lax.dot_general(hidden[:, lower:lower + block_width], down_out[:, lower:lower + block_width], (((1,), (1,)), ((), ())), preferred_element_type=jnp.float32)
        partial_value = lax.optimization_barrier(partial_value.astype(jnp.bfloat16)).astype(jnp.float32)
        running = running + partial_value
    return (running.astype(jnp.bfloat16), gate_out, up_out, down_out)
```

```python
import functools

import jax
import jax.numpy as jnp
from jax import lax
from jax.experimental import pallas as pl
from jax.experimental.pallas import tpu as pltpu
from jax.sharding import PartitionSpec as P

MESH = pl.DeviceIdType.MESH


def normalize(source):
    widened = source.astype(jnp.float32)
    return (widened * lax.rsqrt(jnp.mean(widened * widened, axis=1, keepdims=True) + 1e-06)).astype(
        jnp.bfloat16
    )


def shards(tokens, norm_gain, gate_weight, up_weight, down_weight):
    row_gain = norm_gain[:, None]
    gate_local = (gate_weight * row_gain).astype(jnp.bfloat16)
    up_local = (up_weight * row_gain).astype(jnp.bfloat16)
    down_local = down_weight.astype(jnp.bfloat16)
    normed = normalize(tokens)
    gathered = lax.all_gather(normed, "tp", axis=0, tiled=True)
    down_whole = lax.all_gather(down_local, "fs", axis=0, tiled=True)
    gate_piece = lax.all_gather(gate_local, "fs", axis=0, tiled=True)
    up_piece = lax.all_gather(up_local, "fs", axis=0, tiled=True)
    gate_acc = jnp.dot(gathered, gate_piece, preferred_element_type=jnp.float32)
    up_acc = jnp.dot(gathered, up_piece, preferred_element_type=jnp.float32)
    hidden = (jax.nn.silu(gate_acc) * up_acc).astype(jnp.bfloat16)
    partial_value = lax.dot_general(
        hidden, down_whole, (((1,), (1,)), ((), ())), preferred_element_type=jnp.float32
    )
    mixed_rows = lax.psum_scatter(
        lax.optimization_barrier(partial_value.astype(jnp.bfloat16))
        .astype(jnp.float32)
        .astype(jnp.bfloat16),
        "tp",
        scatter_dimension=0,
        tiled=True,
    )
    return (mixed_rows, gate_piece, up_piece, down_whole)


def kernel(
    Z, TP, tok_ref, gain_ref, gw_ref, uw_ref, dw_ref, mix_ref, g_ref, u_ref, d_ref,
    x_buf, sg_buf, h_buf, part_buf, in_buf,
    zm_sem, zp_sem, y_sem, hp_sem, w_recv, x_send, x_recv, r_send, r_recv,
):
    fs, tp = lax.axis_index("fs"), lax.axis_index("tp")
    z, y = fs // 2, lax.rem(fs, 2)
    oy = 1 - y
    pz = z + 1 - 2 * lax.rem(z, 2)
    R, F = gw_ref.shape
    half = R // 2
    T = tok_ref.shape[0]
    weights = (g_ref, u_ref, d_ref)

    def dev(zz, yy):
        return (zz * 2 + yy, tp)

    def peer(p):
        return lax.rem(tp + p, TP)

    barrier = pltpu.get_barrier_semaphore()

    def greet(target):
        pl.semaphore_signal(barrier, inc=1, device_id=target, device_id_type=MESH)

    greet(dev(z, oy))
    for p in range(1, TP):
        greet((fs, peer(p)))

    @pl.when(z > 0)
    def _():
        greet(dev(z - 1, y))

    @pl.when(z < Z - 1)
    def _():
        greet(dev(z + 1, y))

    gain = gain_ref[...]
    own = pl.ds(pl.multiple_of(fs * R, R), R)
    g_ref[own, :] = (gw_ref[...] * gain).astype(jnp.bfloat16)
    u_ref[own, :] = (uw_ref[...] * gain).astype(jnp.bfloat16)

    pl.semaphore_wait(barrier, TP + jnp.where(z > 0, 1, 0) + jnp.where(z < Z - 1, 1, 0))

    def piece(w, zz, yy, h):
        return weights[w].at[pl.ds(pl.multiple_of((zz * 2 + yy) * R + h * half, half), half), :]

    def move(w, zz, yy, h, sem, target):
        ref = piece(w, zz, yy, h)
        return pltpu.make_async_remote_copy(
            src_ref=ref, dst_ref=ref, send_sem=sem, recv_sem=w_recv.at[w, zz * 2 + yy, h],
            device_id=target, device_id_type=MESH,
        )

    def arrive(w, zz, yy, h):
        move(w, zz, yy, h, hp_sem.at[w], dev(z, oy)).wait_recv()

    def down_z(w, k, h, act):
        @pl.when(jnp.logical_and(z > 0, z + k < Z))
        def _():
            act(move(w, z + k, y, h, zm_sem.at[w, k, h], dev(z - 1, y)))

    def up_z(w, k, h, act):
        @pl.when(jnp.logical_and(z < Z - 1, z - k >= 0))
        def _():
            act(move(w, z - k, y, h, zp_sem.at[w, k, h], dev(z + 1, y)))

    def across(w, zz, h, act):
        @pl.when(jnp.logical_and(zz >= 0, zz < Z))
        def _():
            @pl.when(jnp.logical_or(zz != pz, h != 1))
            def _():
                act(move(w, zz, y, h, y_sem.at[w, zz, h], dev(z, oy)))

    def begin(copy):
        copy.start()

    def finish(copy):
        copy.wait_send()

    def send_own(w):
        for h in range(2):
            down_z(w, 0, h, begin)
            up_z(w, 0, h, begin)
            across(w, z, h, begin)

    def event(w, e):
        d, h = 1 + e // 2, lax.rem(e, 2)
        for sign in (1, -1):
            zz = z + sign * d

            @pl.when(jnp.logical_and(zz >= 0, zz < Z))
            def _():
                arrive(w, zz, y, h)
                (down_z if sign == 1 else up_z)(w, d, h, begin)
                across(w, zz, h, begin)

    def events(w, low, high):
        lax.fori_loop(low, high, lambda e, c: (event(w, e), c)[1], 0)

    def side(w):
        return move(w, z, oy, 1, hp_sem.at[w], dev(pz, y))

    def send_side(w):
        arrive(w, z, oy, 1)
        side(w).start()

    def arrive_other(w, zz):
        arrive(w, zz, oy, 0)

        @pl.when(zz != z)
        def _():
            arrive(w, zz, oy, 1)

    def arrive_rest(w):
        lax.fori_loop(0, Z, lambda zz, c: (arrive_other(w, zz), c)[1], 0)

    last = 2 * (Z - 1)
    send_own(0)
    send_own(1)

    wide = tok_ref[...].astype(jnp.float32)
    x_buf[pl.ds(pl.multiple_of(tp * T, T), T), :] = (
        wide * lax.rsqrt(jnp.mean(wide * wide, axis=1, keepdims=True) + 1e-06)
    ).astype(jnp.bfloat16)
    d_ref[own, :] = dw_ref[...].astype(jnp.bfloat16)

    def rows_to(p, owner):
        ref = x_buf.at[pl.ds(pl.multiple_of(owner * T, T), T), :]
        return pltpu.make_async_remote_copy(
            src_ref=ref, dst_ref=ref, send_sem=x_send.at[p - 1], recv_sem=x_recv.at[p - 1],
            device_id=(fs, peer(p)), device_id_type=MESH,
        )

    for p in range(1, TP):
        rows_to(p, tp).start()

    events(0, 0, 2)
    send_own(2)
    events(0, 2, last)
    send_side(0)

    events(1, 0, 2)
    arrive_rest(0)
    for p in range(1, TP):
        rows_to(p, lax.rem(tp + TP - p, TP)).wait_recv()

    wide_tile = 256
    whole, rest = F // wide_tile, F % wide_tile

    def tiles(body):
        def step(i, c):
            body(pl.ds(pl.multiple_of(i * wide_tile, wide_tile), wide_tile))
            return c

        lax.fori_loop(0, whole, step, 0)
        if rest:
            body(pl.ds(whole * wide_tile, rest))

    def gate_tile(cols):
        v = jnp.dot(x_buf[...], g_ref[:, cols], preferred_element_type=jnp.float32)
        sg_buf[:, cols] = v / (1.0 + jnp.exp(-v))

    def up_tile(cols):
        v = jnp.dot(x_buf[...], u_ref[:, cols], preferred_element_type=jnp.float32)
        h_buf[:, cols] = (sg_buf[:, cols] * v).astype(jnp.bfloat16)

    tiles(gate_tile)
    events(1, 2, last)
    send_side(1)

    events(2, 0, 2)
    arrive_rest(1)
    tiles(up_tile)

    def share(p, s):
        cols = pl.ds(pl.multiple_of(s * R, R), R)
        return pltpu.make_async_remote_copy(
            src_ref=part_buf.at[pl.ds(pl.multiple_of(peer(p) * T, T), T), cols],
            dst_ref=in_buf.at[p - 1, :, cols],
            send_sem=r_send.at[p - 1, s], recv_sem=r_recv.at[p - 1, s],
            device_id=(fs, peer(p)), device_id_type=MESH,
        )

    def unit(zz, yy):
        s = zz * 2 + yy
        span = pl.ds(pl.multiple_of(s * R, R), R)
        part_buf[:, span] = lax.dot_general(
            h_buf[...], d_ref[span, :], (((1,), (1,)), ((), ())), preferred_element_type=jnp.float32
        ).astype(jnp.bfloat16)
        for p in range(1, TP):
            share(p, s).start()

    mirrored = z >= Z // 2
    near_end = jnp.where(mirrored, Z - 1 - z, z)

    def place(i):
        at = jnp.where(i <= near_end, near_end - i, i)
        return jnp.where(mirrored, Z - 1 - at, at)

    def own_row(e, c):
        event(2, e)

        @pl.when(e == last - 1)
        def _():
            send_side(2)

        unit(place(e - 2), y)
        return c

    lax.fori_loop(2, last, own_row, 0)

    def other_row(i, c):
        zz = place(lax.rem(i * 2, Z) + (i * 2) // Z)
        arrive_other(2, zz)
        unit(zz, oy)
        return c

    lax.fori_loop(0, Z, other_row, 0)

    def total(q, c):
        i = q - Z
        s = jnp.where(
            q < Z, place(lax.rem(q, Z)) * 2 + y, place(lax.rem(q * 2, Z) + (i * 2) // Z) * 2 + oy
        )
        cols = pl.ds(pl.multiple_of(s * R, R), R)
        value = part_buf[pl.ds(pl.multiple_of(tp * T, T), T), cols].astype(jnp.float32)
        for p in range(1, TP):
            share(p, s).wait_recv()
            value = value + in_buf[p - 1, :, cols].astype(jnp.float32)
        mix_ref[:, cols] = value.astype(jnp.bfloat16)
        for p in range(1, TP):
            share(p, s).wait_send()
        return c

    lax.fori_loop(0, 2 * Z, total, 0)

    for p in range(1, TP):
        rows_to(p, tp).wait_send()
    for w in range(3):
        side(w).wait_send()

        def drain(q, c):
            k, h = q // 2, lax.rem(q, 2)
            down_z(w, k, h, finish)
            up_z(w, k, h, finish)
            across(w, k, h, finish)
            return c

        lax.fori_loop(0, 2 * Z, drain, 0)


def fused(Z, TP, tokens, norm_gain, gate_weight, up_weight, down_weight):
    T, D = tokens.shape
    R, F = gate_weight.shape
    S = 2 * Z
    whole = jax.ShapeDtypeStruct((R * S, F), jnp.bfloat16)
    vmem = pl.BlockSpec(memory_space=pltpu.VMEM)
    dma = pltpu.SemaphoreType.DMA
    return pl.pallas_call(
        functools.partial(kernel, Z, TP),
        out_shape=(jax.ShapeDtypeStruct((T, D), jnp.bfloat16), whole, whole, whole),
        in_specs=[vmem] * 5,
        out_specs=(vmem,) * 4,
        scratch_shapes=[
            pltpu.VMEM((T * TP, D), jnp.bfloat16),
            pltpu.VMEM((T * TP, F), jnp.float32),
            pltpu.VMEM((T * TP, F), jnp.bfloat16),
            pltpu.VMEM((T * TP, D), jnp.bfloat16),
            pltpu.VMEM((TP - 1, T, D), jnp.bfloat16),
            dma((3, Z, 2)),
            dma((3, Z, 2)),
            dma((3, Z, 2)),
            dma((3,)),
            dma((3, S, 2)),
            dma((TP - 1,)),
            dma((TP - 1,)),
            dma((TP - 1, S)),
            dma((TP - 1, S)),
        ],
        compiler_params=pltpu.CompilerParams(
            collective_id=0, has_side_effects=True, vmem_limit_bytes=60 * 1024 * 1024
        ),
    )(tokens, norm_gain[:, None], gate_weight, up_weight, down_weight)


def solution(mesh):
    in_specs = (P(("fs", "tp"), None), P("fs"), P("fs", "tp"), P("fs", "tp"), P("fs", "tp"))
    out_specs = (P(("fs", "tp"), None), P(None, "tp"), P(None, "tp"), P(None, "tp"))
    Z, TP = mesh.shape["fs"] // 2, mesh.shape["tp"]

    def step(tokens, norm_gain, gate_weight, up_weight, down_weight):
        args = (tokens, norm_gain, gate_weight, up_weight, down_weight)
        if mesh.shape["fs"] == 2 * TP == 8 and gate_weight.shape[1] % 128 == 0:
            return fused(Z, TP, *args)
        return shards(*args)

    return jax.shard_map(step, mesh=mesh, in_specs=in_specs, out_specs=out_specs, check_vma=False)
```

```python
import functools

import jax
import jax.numpy as jnp
from jax import lax
from jax.experimental import pallas as pl
from jax.experimental.pallas import tpu as pltpu
from jax.sharding import PartitionSpec as P

MESH = pl.DeviceIdType.MESH
N = 2


def normalize(source):
    widened = source.astype(jnp.float32)
    return (widened * lax.rsqrt(jnp.mean(widened * widened, axis=1, keepdims=True) + 1e-06)).astype(
        jnp.bfloat16
    )


def shards(tokens, norm_gain, gate_weight, up_weight, down_weight):
    row_gain = norm_gain[:, None]
    gate_local = (gate_weight * row_gain).astype(jnp.bfloat16)
    up_local = (up_weight * row_gain).astype(jnp.bfloat16)
    down_local = down_weight.astype(jnp.bfloat16)
    normed = normalize(tokens)
    gathered = lax.all_gather(normed, "tp", axis=0, tiled=True)
    down_whole = lax.all_gather(down_local, "fs", axis=0, tiled=True)
    gate_piece = lax.all_gather(gate_local, "fs", axis=0, tiled=True)
    up_piece = lax.all_gather(up_local, "fs", axis=0, tiled=True)
    gate_acc = jnp.dot(gathered, gate_piece, preferred_element_type=jnp.float32)
    up_acc = jnp.dot(gathered, up_piece, preferred_element_type=jnp.float32)
    hidden = (jax.nn.silu(gate_acc) * up_acc).astype(jnp.bfloat16)
    partial_value = lax.dot_general(
        hidden, down_whole, (((1,), (1,)), ((), ())), preferred_element_type=jnp.float32
    )
    mixed_rows = lax.psum_scatter(
        lax.optimization_barrier(partial_value.astype(jnp.bfloat16))
        .astype(jnp.float32)
        .astype(jnp.bfloat16),
        "tp",
        scatter_dimension=0,
        tiled=True,
    )
    return (mixed_rows, gate_piece, up_piece, down_whole)


def kernel(
    Z, TP, tok_ref, gain_ref, gw_ref, uw_ref, dw_ref, mix_ref, g_ref, u_ref, d_ref,
    x_buf, sg_buf, h_buf, part_buf, in_buf,
    zm_sem, zp_sem, y_sem, hp_sem, w_recv, x_send, x_recv, r_send, r_recv,
):
    fs, tp = lax.axis_index("fs"), lax.axis_index("tp")
    z, y = fs // 2, lax.rem(fs, 2)
    oy = 1 - y
    pz = z + 1 - 2 * lax.rem(z, 2)
    R, F = gw_ref.shape
    half = R // N
    T = tok_ref.shape[0]
    weights = (g_ref, u_ref, d_ref)

    def dev(zz, yy):
        return (zz * 2 + yy, tp)

    def peer(p):
        return lax.rem(tp + p, TP)

    barrier = pltpu.get_barrier_semaphore()

    def greet(target):
        pl.semaphore_signal(barrier, inc=1, device_id=target, device_id_type=MESH)

    greet(dev(z, oy))
    for p in range(1, TP):
        greet((fs, peer(p)))

    @pl.when(z > 0)
    def _():
        greet(dev(z - 1, y))

    @pl.when(z < Z - 1)
    def _():
        greet(dev(z + 1, y))

    gain = jnp.broadcast_to(gain_ref[...], (128, R)).T[:, :1]
    own = pl.ds(pl.multiple_of(fs * R, R), R)
    g_ref[own, :] = (gw_ref[...] * gain).astype(jnp.bfloat16)
    u_ref[own, :] = (uw_ref[...] * gain).astype(jnp.bfloat16)

    pl.semaphore_wait(barrier, TP + jnp.where(z > 0, 1, 0) + jnp.where(z < Z - 1, 1, 0))

    def piece(w, zz, yy, h):
        return weights[w].at[pl.ds(pl.multiple_of((zz * 2 + yy) * R + h * half, half), half), :]

    def move(w, zz, yy, h, sem, target):
        ref = piece(w, zz, yy, h)
        return pltpu.make_async_remote_copy(
            src_ref=ref, dst_ref=ref, send_sem=sem, recv_sem=w_recv.at[w, zz * 2 + yy, h],
            device_id=target, device_id_type=MESH,
        )

    def arrive(w, zz, yy, h):
        move(w, zz, yy, h, hp_sem.at[w, 0], dev(z, oy)).wait_recv()

    def down_z(w, k, h, act):
        @pl.when(jnp.logical_and(z > 0, z + k < Z))
        def _():
            act(move(w, z + k, y, h, zm_sem.at[w, k, h], dev(z - 1, y)))

    def up_z(w, k, h, act):
        @pl.when(jnp.logical_and(z < Z - 1, z - k >= 0))
        def _():
            act(move(w, z - k, y, h, zp_sem.at[w, k, h], dev(z + 1, y)))

    def across(w, zz, h, act):
        @pl.when(jnp.logical_and(zz >= 0, zz < Z))
        def _():
            @pl.when(jnp.logical_or(zz != pz, h < N // 2))
            def _():
                act(move(w, zz, y, h, y_sem.at[w, zz, h], dev(z, oy)))

    def begin(copy):
        copy.start()

    def finish(copy):
        copy.wait_send()

    def send_own(w):
        for h in range(N):
            down_z(w, 0, h, begin)
            up_z(w, 0, h, begin)
            across(w, z, h, begin)

    def event(w, e):
        d, h = 1 + e // N, lax.rem(e, N)
        for sign in (1, -1):
            zz = z + sign * d

            @pl.when(jnp.logical_and(zz >= 0, zz < Z))
            def _():
                arrive(w, zz, y, h)
                (down_z if sign == 1 else up_z)(w, d, h, begin)
                across(w, zz, h, begin)

    def events(w, low, high):
        lax.fori_loop(low, high, lambda e, c: (event(w, e), c)[1], 0)

    def side(w, h):
        return move(w, z, oy, h, hp_sem.at[w, h - N // 2], dev(pz, y))

    def send_side(w):
        for h in range(N // 2, N):
            arrive(w, z, oy, h)
            side(w, h).start()

    def arrive_other(w, zz):
        for h in range(N // 2):
            arrive(w, zz, oy, h)

        @pl.when(zz != z)
        def _():
            for h in range(N // 2, N):
                arrive(w, zz, oy, h)

    def arrive_rest(w):
        lax.fori_loop(0, Z, lambda zz, c: (arrive_other(w, zz), c)[1], 0)

    last = N * (Z - 1)
    send_own(0)
    send_own(1)

    wide = tok_ref[...].astype(jnp.float32)
    x_buf[pl.ds(pl.multiple_of(tp * T, T), T), :] = (
        wide * lax.rsqrt(jnp.mean(wide * wide, axis=1, keepdims=True) + 1e-06)
    ).astype(jnp.bfloat16)
    d_ref[own, :] = dw_ref[...].astype(jnp.bfloat16)

    def rows_to(p, owner):
        ref = x_buf.at[pl.ds(pl.multiple_of(owner * T, T), T), :]
        return pltpu.make_async_remote_copy(
            src_ref=ref, dst_ref=ref, send_sem=x_send.at[p - 1], recv_sem=x_recv.at[p - 1],
            device_id=(fs, peer(p)), device_id_type=MESH,
        )

    for p in range(1, TP):
        rows_to(p, tp).start()

    events(0, 0, N)
    send_own(2)
    events(0, N, last)
    send_side(0)

    events(1, 0, N)
    arrive_rest(0)
    for p in range(1, TP):
        rows_to(p, lax.rem(tp + TP - p, TP)).wait_recv()

    wide_tile = 256
    whole, rest = F // wide_tile, F % wide_tile

    def tiles(body):
        def step(i, c):
            body(pl.ds(pl.multiple_of(i * wide_tile, wide_tile), wide_tile))
            return c

        lax.fori_loop(0, whole, step, 0)
        if rest:
            body(pl.ds(whole * wide_tile, rest))

    def gate_tile(cols):
        v = jnp.dot(x_buf[...], g_ref[:, cols], preferred_element_type=jnp.float32)
        sg_buf[:, cols] = v / (1.0 + jnp.exp(-v))

    def up_tile(cols):
        v = jnp.dot(x_buf[...], u_ref[:, cols], preferred_element_type=jnp.float32)
        h_buf[:, cols] = (sg_buf[:, cols] * v).astype(jnp.bfloat16)

    tiles(gate_tile)
    events(1, N, last)
    send_side(1)

    events(2, 0, N)
    arrive_rest(1)
    tiles(up_tile)

    def span(zz, yy, h):
        return pl.ds(pl.multiple_of((zz * 2 + yy) * R + h * half, half), half)

    def share(p, zz, yy, h):
        cols = span(zz, yy, h)
        s = zz * 2 + yy
        return pltpu.make_async_remote_copy(
            src_ref=part_buf.at[pl.ds(pl.multiple_of(peer(p) * T, T), T), cols],
            dst_ref=in_buf.at[p - 1, :, cols],
            send_sem=r_send.at[p - 1, s, h], recv_sem=r_recv.at[p - 1, s, h],
            device_id=(fs, peer(p)), device_id_type=MESH,
        )

    def unit(zz, yy, h):
        cols = span(zz, yy, h)
        part_buf[:, cols] = lax.dot_general(
            h_buf[...], d_ref[cols, :], (((1,), (1,)), ((), ())), preferred_element_type=jnp.float32
        ).astype(jnp.bfloat16)
        for p in range(1, TP):
            share(p, zz, yy, h).start()

    mirrored = z >= Z // 2
    near_end = jnp.where(mirrored, Z - 1 - z, z)

    def place(i):
        at = jnp.where(i <= near_end, near_end - i, i)
        return jnp.where(mirrored, Z - 1 - at, at)

    def own_row(e, c):
        event(2, e)

        @pl.when(e == last - 1)
        def _():
            send_side(2)

        @pl.when(lax.rem(e, N // 2) == N // 2 - 1)
        def _():
            def piece_of(h, c):
                unit(place((e - N) // (N // 2)), y, h)
                return c

            lax.fori_loop(0, N, piece_of, 0)

        return c

    lax.fori_loop(N, last, own_row, 0)

    def other(q):
        early, pairs = q < Z * N // 2, Z // 2
        left = q - Z * N // 2
        i = jnp.where(early, q // N * 2, 1 + lax.rem(left + pairs * N, pairs) * 2)
        h = jnp.where(early, lax.rem(q, N), (left + pairs * N) // pairs - N)
        return place(i), h

    def other_row(q, c):
        zz, h = other(q)

        @pl.when(jnp.logical_or(zz != z, h < N // 2))
        def _():
            arrive(2, zz, oy, h)

        unit(zz, oy, h)
        return c

    lax.fori_loop(0, Z * N, other_row, 0)

    def total(zz, yy, h):
        cols = span(zz, yy, h)
        value = part_buf[pl.ds(pl.multiple_of(tp * T, T), T), cols].astype(jnp.float32)
        for p in range(1, TP):
            share(p, zz, yy, h).wait_recv()
            value = value + in_buf[p - 1, :, cols].astype(jnp.float32)
        mix_ref[:, cols] = value.astype(jnp.bfloat16)
        for p in range(1, TP):
            share(p, zz, yy, h).wait_send()

    def total_own(q, c):
        total(place(q // N), y, lax.rem(q, N))
        return c

    def total_other(q, c):
        zz, h = other(q)
        total(zz, oy, h)
        return c

    lax.fori_loop(0, Z * N, total_own, 0)
    lax.fori_loop(0, Z * N, total_other, 0)

    for p in range(1, TP):
        rows_to(p, tp).wait_send()
    for w in range(3):
        for h in range(N // 2, N):
            side(w, h).wait_send()

        def drain(q, c):
            k, h = q // N, lax.rem(q, N)
            down_z(w, k, h, finish)
            up_z(w, k, h, finish)
            across(w, k, h, finish)
            return c

        lax.fori_loop(0, N * Z, drain, 0)


def store(*refs):
    sems = refs[8]
    copies = [pltpu.make_async_copy(refs[i], refs[4 + i], sems.at[i]) for i in range(4)]
    for copy in copies:
        copy.start()
    for copy in copies:
        copy.wait()


def fused(Z, TP, tokens, norm_gain, gate_weight, up_weight, down_weight):
    T, D = tokens.shape
    R, F = gate_weight.shape
    S = 2 * Z
    whole = pltpu.VMEM((R * S, F), jnp.bfloat16)
    vmem = pl.BlockSpec(memory_space=pltpu.VMEM)
    dma = pltpu.SemaphoreType.DMA
    results = pl.pallas_call(
        functools.partial(kernel, Z, TP),
        out_shape=(pltpu.VMEM((T, D), jnp.bfloat16), whole, whole, whole),
        in_specs=[vmem] * 5,
        out_specs=(vmem,) * 4,
        scratch_shapes=[
            pltpu.VMEM((T * TP, D), jnp.bfloat16),
            pltpu.VMEM((T * TP, F), jnp.float32),
            pltpu.VMEM((T * TP, F), jnp.bfloat16),
            pltpu.VMEM((T * TP, D), jnp.bfloat16),
            pltpu.VMEM((TP - 1, T, D), jnp.bfloat16),
            dma((3, Z, N)),
            dma((3, Z, N)),
            dma((3, Z, N)),
            dma((3, N // 2)),
            dma((3, S, N)),
            dma((TP - 1,)),
            dma((TP - 1,)),
            dma((TP - 1, S, N)),
            dma((TP - 1, S, N)),
        ],
        compiler_params=pltpu.CompilerParams(
            collective_id=0, has_side_effects=True, vmem_limit_bytes=36 * 1024 * 1024
        ),
    )(tokens, norm_gain[None, :], gate_weight, up_weight, down_weight)
    return pl.pallas_call(
        store,
        out_shape=[jax.ShapeDtypeStruct(r.shape, r.dtype) for r in results],
        in_specs=[vmem] * 4,
        out_specs=[pl.BlockSpec(memory_space=pl.ANY)] * 4,
        scratch_shapes=[dma((4,))],
        compiler_params=pltpu.CompilerParams(vmem_limit_bytes=1024 * 1024),
    )(*results)


def solution(mesh):
    in_specs = (P(("fs", "tp"), None), P("fs"), P("fs", "tp"), P("fs", "tp"), P("fs", "tp"))
    out_specs = (P(("fs", "tp"), None), P(None, "tp"), P(None, "tp"), P(None, "tp"))
    Z, TP = mesh.shape["fs"] // 2, mesh.shape["tp"]

    def step(tokens, norm_gain, gate_weight, up_weight, down_weight):
        args = (tokens, norm_gain, gate_weight, up_weight, down_weight)
        if mesh.shape["fs"] == 2 * TP == 8 and gate_weight.shape[1] % 128 == 0:
            return fused(Z, TP, *args)
        return shards(*args)

    return jax.shard_map(step, mesh=mesh, in_specs=in_specs, out_specs=out_specs, check_vma=False)
```
